32 devices in a mesh: fs: 8 (over z, x), tp: 4 (over y, core).
Axes of the slice: x: 2, y: 2, z: 4, core: 2. Of those that a mesh axis runs over, the one named last changes fastest.
Arguments:
- tokens: bfloat16 [8192, 2048], P(('fs', 'tp')), may hold values from -6 to 6
- mix_gain: float32 [2048], replicated, may hold values from 0.1 to 1.9
- ffn_gain: float32 [2048], replicated, may hold values from 0.1 to 1.9
- u_weight: float32 [2048, 2048], P('fs', 'tp'), may hold values from -0.125 to 0.125
- u_scale: float32 [2048], P('tp'), may hold values from 0.5 to 2
- v_weight: float32 [2048, 2048], P('fs', 'tp'), may hold values from -0.125 to 0.125
- v_scale: float32 [2048], P('tp'), may hold values from 0.3 to 12
- v_gain: float32 [2048], P('tp'), may hold values from 0.1 to 1.9
- spatial_weight: bfloat16 [8, 128, 128], replicated, may hold values from -0.5 to 0.5
- spatial_bias: float32 [8, 128], replicated, may hold values from 0.1 to 1.9
- out_weight: float32 [2048, 2048], P('tp', 'fs'), may hold values from -0.125 to 0.125
- out_scale: float32 [2048], P('fs'), may hold values from 0.5 to 2
- gate_weight: float32 [2048, 6144], P('fs', 'tp'), may hold values from -0.125 to 0.125
- gate_scale: float32 [6144], P('tp'), may hold values from 0.5 to 2
- up_weight: float32 [2048, 6144], P('fs', 'tp'), may hold values from -0.125 to 0.125
- up_scale: float32 [6144], P('tp'), may hold values from 0.5 to 2
- down_weight: float32 [6144, 2048], P('tp', 'fs'), may hold values from -0.078125 to 0.078125
- down_scale: float32 [2048], P('fs'), may hold values from 0.5 to 2
Outputs:
- layer_out: bfloat16 [8192, 2048], P(('fs', 'tp'))
The draws below stay inside these ranges and needn't reach their ends.
All inputs are finite; a program needn't handle non-finite values.
Results may differ from the reference program's by a relative error of at most 0.02.
Values may be sent and summed in bfloat16 or wider, within the bound.
A program may use at most 128 MiB of HBM per device.

```python
import math
import jax
import jax.numpy as jnp
from jax import lax

D = 2048
A = 2048
A_GROUPS = 8
BLK = 128
FF = 6144
TOKENS = 8192
N_TP = 4


def draw_v_scale(key, part):
    column_ramp = jnp.arange(A, dtype=jnp.float32) / A
    base_scale = jnp.exp(jax.random.uniform(key, (A,), jnp.float32, math.log(0.3), math.log(3.0)))
    return base_scale * 3.0 ** column_ramp


def block_levels(key, dims, split, low, largest):
    loudness, own = 1.0, jax.random.fold_in(key, 6)
    for dim, parts in split:
        heights = jnp.exp(jax.random.uniform(jax.random.fold_in(own, dim), (parts,), jnp.float32, low / len(split), largest / len(split)))
        loudness = loudness * jnp.repeat(heights, dims[dim] // parts).reshape([-1 if axis == dim else 1 for axis in range(len(dims))])
    return loudness


def centred(rng, dims, scale, reach, pieces=(), held_as=jnp.bfloat16):
    factor_of = block_levels(rng, dims, pieces, -0.22, 0.18) if pieces else 1.0
    entries = jax.random.normal(rng, dims, jnp.float32) * scale * factor_of
    return jnp.minimum(jnp.maximum(entries, -reach), reach).astype(held_as)


def setup_inputs(seed: int = 0) -> dict:
    keys = jax.random.split(jax.random.key(seed), 19)
    tokens = centred(keys[0], (TOKENS, D), 1.0, 6.0, ((0, 32),))
    mix_gain = jnp.clip(1.0 + 0.18 * jax.random.normal(keys[1], (D,), jnp.float32), 0.1, 1.9)
    ffn_gain = jnp.clip(1.0 + 0.18 * jax.random.normal(keys[2], (D,), jnp.float32), 0.1, 1.9)
    u_weight = centred(keys[3], (D, A), D ** -0.5, 0.125, ((0, 8), (1, 4)), jnp.float32)
    u_scale = jnp.clip(jnp.exp(math.log(2.0) - 1.3862944 * jax.random.uniform(keys[4], (A,), jnp.float32) ** block_levels(keys[4], (A,), ((0, 4),), -0.2, 0.2)), 0.5, 2.0)
    v_weight = centred(keys[5], (D, A), D ** -0.5, 0.125, ((0, 8), (1, 4)), jnp.float32)
    v_scale = draw_v_scale(jax.random.fold_in(keys[18], 71), 0)
    v_gain = jnp.clip(1.0 + 0.18 * jax.random.normal(keys[7], (A,), jnp.float32), 0.1, 1.9)
    spatial_weight = centred(keys[8], (A_GROUPS, BLK, BLK), BLK ** -0.5, 0.5)
    spatial_bias = jnp.clip(1.0 + 0.18 * jax.random.normal(keys[9], (A_GROUPS, BLK), jnp.float32), 0.1, 1.9)
    out_weight = centred(keys[10], (A, D), A ** -0.5, 0.125, ((0, 4), (1, 8)), jnp.float32)
    out_scale = jnp.clip(jnp.exp(math.log(2.0) - 1.3862944 * jax.random.uniform(keys[11], (D,), jnp.float32) ** block_levels(keys[11], (D,), ((0, 8),), -0.2, 0.2)), 0.5, 2.0)
    gate_weight = centred(keys[12], (D, FF), D ** -0.5, 0.125, ((0, 8), (1, 4)), jnp.float32)
    gate_scale = jnp.clip(jnp.exp(math.log(2.0) - 1.3862944 * jax.random.uniform(keys[13], (FF,), jnp.float32) ** block_levels(keys[13], (FF,), ((0, 4),), -0.2, 0.2)), 0.5, 2.0)
    up_weight = centred(keys[14], (D, FF), D ** -0.5, 0.125, ((0, 8), (1, 4)), jnp.float32)
    up_scale = jnp.clip(jnp.exp(math.log(2.0) - 1.3862944 * jax.random.uniform(keys[15], (FF,), jnp.float32) ** block_levels(keys[15], (FF,), ((0, 4),), -0.2, 0.2)), 0.5, 2.0)
    down_weight = centred(keys[16], (FF, D), FF ** -0.5, 0.078125, ((0, 4), (1, 8)), jnp.float32)
    down_scale = jnp.clip(jnp.exp(math.log(2.0) - 1.3862944 * jax.random.uniform(keys[17], (D,), jnp.float32) ** block_levels(keys[17], (D,), ((0, 8),), -0.2, 0.2)), 0.5, 2.0)
    return {"tokens": tokens, "mix_gain": mix_gain, "ffn_gain": ffn_gain, "u_weight": u_weight, "u_scale": u_scale, "v_weight": v_weight, "v_scale": v_scale, "v_gain": v_gain, "spatial_weight": spatial_weight, "spatial_bias": spatial_bias, "out_weight": out_weight, "out_scale": out_scale, "gate_weight": gate_weight, "gate_scale": gate_scale, "up_weight": up_weight, "up_scale": up_scale, "down_weight": down_weight, "down_scale": down_scale}


def rms_rows(values, norm_gain):
    widened = values.astype(jnp.float32)
    factor = lax.rsqrt(lax.optimization_barrier(jnp.mean(widened * widened, axis=1, keepdims=True)) + 1e-06)
    return (widened * factor * norm_gain).astype(jnp.bfloat16)

def project(values, matrix, scales):
    return jnp.dot(values, matrix.astype(jnp.bfloat16), preferred_element_type=jnp.float32) * scales

def run_sums(values, matrix, scales):
    run_length = values.shape[1] // N_TP
    narrow = matrix.astype(jnp.bfloat16)
    summed = jnp.zeros((values.shape[0], matrix.shape[1]), jnp.float32)
    for run_index in range(N_TP):
        lower = run_index * run_length
        partial_value = jnp.dot(values[:, lower:lower + run_length], narrow[lower:lower + run_length], preferred_element_type=jnp.float32) * scales
        summed = summed + lax.optimization_barrier(partial_value.astype(jnp.bfloat16)).astype(jnp.float32)
    return summed

def reference(tokens, mix_gain, ffn_gain, u_weight, u_scale, v_weight, v_scale, v_gain, spatial_weight, spatial_bias, out_weight, out_scale, gate_weight, gate_scale, up_weight, up_scale, down_weight, down_scale):
    normed = rms_rows(tokens, mix_gain)
    u_values = jax.nn.gelu(project(normed, u_weight, u_scale), approximate=True).astype(jnp.bfloat16)
    v_values = jax.nn.gelu(project(normed, v_weight, v_scale), approximate=True).astype(jnp.bfloat16)
    v_wide = v_values.astype(jnp.float32)
    average = lax.optimization_barrier(jnp.mean(v_wide, axis=1, keepdims=True))
    spread = lax.optimization_barrier(jnp.mean(v_wide * v_wide, axis=1, keepdims=True)) - average * average
    v_normed = ((v_wide - average) * lax.rsqrt(spread + 1e-05) * v_gain).astype(jnp.bfloat16)
    group_dim = A // A_GROUPS
    blocks = v_normed.reshape(TOKENS // BLK, BLK, A_GROUPS, group_dim).astype(jnp.float32)
    causal = jnp.tril(jnp.ones((BLK, BLK), dtype=bool))
    masked = jnp.where(causal[None], spatial_weight, jnp.zeros_like(spatial_weight)).astype(jnp.float32)
    mixed_sum = jnp.einsum('gts,bsgd->btgd', masked, blocks) + spatial_bias.T[None, :, :, None]
    gated_rows = (u_values.reshape(blocks.shape).astype(jnp.float32) * mixed_sum).astype(jnp.bfloat16)
    gated_rows = gated_rows.reshape(TOKENS, A)
    residual = (tokens.astype(jnp.float32) + run_sums(gated_rows, out_weight, out_scale)).astype(jnp.bfloat16)
    normed_second = rms_rows(residual, ffn_gain)
    hidden = (jax.nn.silu(project(normed_second, gate_weight, gate_scale)) * project(normed_second, up_weight, up_scale)).astype(jnp.bfloat16)
    return (residual.astype(jnp.float32) + run_sums(hidden, down_weight, down_scale)).astype(jnp.bfloat16)
```

```python
import functools
import jax
import jax.numpy as jnp
from jax import lax
from jax.experimental import pallas as pl
from jax.experimental.pallas import tpu as pltpu
from jax.sharding import PartitionSpec as P

A_GROUPS = 8
BLK = 128
UV, OUT, GATE, UP, DOWN = range(5)
BF = jnp.bfloat16
F32 = jnp.float32


def rms(values, gain):
    wide = values.astype(F32)
    factor = lax.rsqrt(jnp.mean(wide * wide, axis=1, keepdims=True) + 1e-06)
    return (wide * factor * gain).astype(BF)


def kernel(
    nf, nt, nz, nx,
    tokens, mix_gain, ffn_gain, uv_scale, v_gain, mixers, offsets, gate_scale, up_scale,
    uv_in, out_in, gate_in, up_in, down_in,
    result,
    w_uv, w_out, w_gate, w_up, w_down, rows_all, uvals, vvals, gated, hidden,
    staged, landed, stats, residual,
    own_sem, w_recv, w_send, row_recv, row_send, stat_recv, stat_send, part_recv, part_send,
):
    fs, tp = lax.axis_index("fs"), lax.axis_index("tp")
    coord = {"z": fs // nx, "x": fs % nx}
    size = {"z": nz, "x": nx}
    stride = {"z": nx, "x": 1}
    order = {m: ("z", "x") for m in range(5)}
    local = tokens.shape[0]
    total = rows_all.shape[0]
    width = tokens.shape[1]
    cols = uvals.shape[1]
    sources = (uv_in, out_in, gate_in, up_in, down_in)
    whole = (w_uv, w_out, w_gate, w_up, w_down)

    def slot(m, s):
        if m in (OUT, DOWN):
            return whole[m].at[s]
        depth = sources[m].shape[0]
        return whole[m].at[pl.ds(pl.multiple_of(s * depth, depth), depth)]

    def reaches(axis, d):
        return coord[axis] + d < size[axis] if d > 0 else coord[axis] > 0

    pending = []

    def copy_of(m, s, axis, d):
        lane = (0 if axis == "z" else 2) + (0 if d > 0 else 1)
        return pltpu.make_async_remote_copy(
            src_ref=slot(m, s), dst_ref=slot(m, s),
            send_sem=w_send.at[m, s, lane], recv_sem=w_recv.at[m, s],
            device_id={"fs": fs + d * stride[axis], "tp": tp},
            device_id_type=pl.DeviceIdType.MESH,
        )

    def send(m, s, axis, d, valid):
        allowed = jnp.logical_and(valid, reaches(axis, d))

        @pl.when(allowed)
        def _():
            copy_of(m, s, axis, d).start()

        pending.append((allowed, m, s, axis, d))

    def own(m, axis):
        if size[axis] > 1:
            for d in (1, -1):
                send(m, fs, axis, d, fs >= 0)

    def arrived(m, s, axis, d, valid):
        @pl.when(valid)
        def _():
            copy_of(m, s, axis, -d).wait_recv()

    def first_line(m, then=None):
        p, q = order[m]
        for t in range(1, size[p]):
            for d in (1, -1):
                at = coord[p] - d * t
                valid = jnp.logical_and(at >= 0, at < size[p])
                s = jnp.where(valid, fs - d * t * stride[p], fs)
                arrived(m, s, p, d, valid)
                if t < size[p] - 1:
                    send(m, s, p, d, valid)
                if size[q] > 1:
                    for e in (1, -1):
                        send(m, s, q, e, valid)
                if then:
                    pl.when(valid)(functools.partial(then, s))

    def second_line(m, then=None):
        p, q = order[m]
        for k in range(size[p]):
            for sign in (1, -1) if k else (1,):
                there = coord[p] + sign * k
                inside = jnp.logical_and(there >= 0, there < size[p])
                for t in range(1, size[q]):
                    for d in (1, -1):
                        at = coord[q] - d * t
                        valid = jnp.logical_and(inside, jnp.logical_and(at >= 0, at < size[q]))
                        s = jnp.where(valid, fs + sign * k * stride[p] - d * t * stride[q], fs)
                        arrived(m, s, q, d, valid)
                        if t < size[q] - 1:
                            send(m, s, q, d, valid)
                        if then:
                            pl.when(valid)(functools.partial(then, s))

    mine = [pltpu.make_async_copy(sources[m], slot(m, fs), own_sem.at[m]) for m in range(5)]
    for copy in mine:
        copy.start()
    mine[UV].wait()
    own(UV, "z")
    own(UV, "x")

    def peer_of(j):
        return lax.rem(tp + j, nt)

    def row_copy(phase, j, owner):
        part = rows_all.at[pl.ds(pl.multiple_of(owner * local, local), local)]
        return pltpu.make_async_remote_copy(
            src_ref=part, dst_ref=part,
            send_sem=row_send.at[phase, j], recv_sem=row_recv.at[phase, owner],
            device_id={"fs": fs, "tp": peer_of(j)}, device_id_type=pl.DeviceIdType.MESH,
        )

    def stat_copy(j, owner):
        return pltpu.make_async_remote_copy(
            src_ref=stats.at[owner], dst_ref=stats.at[owner],
            send_sem=stat_send.at[j], recv_sem=stat_recv.at[owner],
            device_id={"fs": fs, "tp": peer_of(j)}, device_id_type=pl.DeviceIdType.MESH,
        )

    def part_copy(phase, j, owner, s):
        peer = peer_of(j)
        return pltpu.make_async_remote_copy(
            src_ref=staged.at[s, pl.ds(pl.multiple_of(peer * local, local), local)],
            dst_ref=landed.at[owner, s],
            send_sem=part_send.at[phase, j, s], recv_sem=part_recv.at[phase, owner, s],
            device_id={"fs": fs, "tp": peer}, device_id_type=pl.DeviceIdType.MESH,
        )

    step = min(64, local)

    def norm_rows(source, gain):
        @pl.loop(0, local // step)
        def _(i):
            here = pl.ds(pl.multiple_of(i * step, step), step)
            there = pl.ds(pl.multiple_of(tp * local + i * step, step), step)
            rows_all[there, :] = rms(source[here, :], gain[...])

    norm_rows(tokens, mix_gain)
    for j in range(1, nt):
        row_copy(0, j, tp).start()
    mine[OUT].wait()
    own(OUT, "x")
    own(OUT, "z")
    mine[GATE].wait()
    own(GATE, "x")
    first_line(UV)
    own(GATE, "z")
    mine[UP].wait()
    own(UP, "x")
    second_line(UV)
    for j in range(1, nt):
        row_copy(0, j, peer_of(j)).wait_recv()

    tile = 256
    stat_rows = BLK

    @pl.loop(0, total // tile)
    def _(i):
        here = pl.ds(pl.multiple_of(i * tile, tile), tile)
        for c in range(2 * cols // tile):
            at = slice(c * tile, (c + 1) * tile)
            pre = jnp.dot(rows_all[here, :], w_uv[:, at], preferred_element_type=F32)
            value = jax.nn.gelu(pre * uv_scale[:, at], approximate=True).astype(BF)
            if c * tile < cols:
                uvals[here, at] = value
            else:
                vvals[here, c * tile - cols:(c + 1) * tile - cols] = value

    lanes = lax.broadcasted_iota(jnp.int32, (stat_rows, 128), 1)

    @pl.loop(0, total // stat_rows)
    def _(i):
        here = pl.ds(pl.multiple_of(i * stat_rows, stat_rows), stat_rows)
        wide = vvals[here, :].astype(F32)
        sums = jnp.sum(wide, axis=1, keepdims=True)
        squares = jnp.sum(wide * wide, axis=1, keepdims=True)
        both = jnp.where(lanes == 0, sums, jnp.where(lanes == 1, squares, 0.0))
        stats[tp, :, here] = both.T[0:8, :]

    for j in range(1, nt):
        stat_copy(j, tp).start()
    first_line(OUT)
    own(UP, "z")
    mine[DOWN].wait()
    own(DOWN, "x")
    second_line(OUT)
    for j in range(1, nt):
        stat_copy(j, peer_of(j)).wait_recv()

    group_dim = (cols * nt) // A_GROUPS

    @pl.loop(0, total // BLK)
    def _(i):
        here = pl.ds(pl.multiple_of(i * BLK, BLK), BLK)
        summed = stats[0, :, here]
        for t in range(1, nt):
            summed = summed + stats[t, :, here]
        turned = jnp.concatenate([summed] * (BLK // 8), axis=0).T
        average = turned[:, 0:1] / (cols * nt)
        spread = turned[:, 1:2] / (cols * nt) - average * average
        wide = vvals[here, :].astype(F32)
        normed = ((wide - average) * lax.rsqrt(spread + 1e-05) * v_gain[...]).astype(BF)
        for g in range(cols // group_dim):
            at = slice(g * group_dim, (g + 1) * group_dim)
            mixed = jnp.dot(mixers[g], normed[:, at], preferred_element_type=F32)
            mixed = mixed + offsets[:, g:g + 1]
            gated[here, at] = (uvals[here, at].astype(F32) * mixed).astype(BF)

    def product(phase, left, matrix, s):
        part = min(512, total)

        @pl.loop(0, total // part)
        def _(i):
            here = pl.ds(pl.multiple_of(i * part, part), part)
            staged[s, here, :] = jnp.dot(
                left[here, :], matrix[s], preferred_element_type=F32
            ).astype(BF)

        for j in range(1, nt):
            part_copy(phase, j, tp, s).start()

    @pl.loop(0, nf)
    def _(s):
        product(0, gated, w_out, s)

    first_line(GATE)
    own(DOWN, "z")

    block = staged.shape[2]

    def collect(phase, base, target):
        for s in range(nf):
            for j in range(1, nt):
                part_copy(phase, j, peer_of(j), s).wait_recv()
            at = slice(s * block, (s + 1) * block)
            summed = staged[s, pl.ds(pl.multiple_of(tp * local, local), local), :].astype(F32)
            for j in range(1, nt):
                summed = summed + landed[peer_of(j), s].astype(F32)
            target[:, at] = (base[:, at].astype(F32) + summed).astype(BF)

    collect(0, tokens, residual)
    for j in range(1, nt):
        row_copy(0, j, tp).wait_send()
    norm_rows(residual, ffn_gain)
    for j in range(1, nt):
        row_copy(1, j, tp).start()

    @pl.loop(0, nf)
    def _(s):
        for j in range(1, nt):
            part_copy(0, j, tp, s).wait_send()

    first_line(UP)
    second_line(GATE)
    for j in range(1, nt):
        row_copy(1, j, peer_of(j)).wait_recv()
    first_line(DOWN)
    second_line(UP)
    hidden_cols = hidden.shape[1]

    @pl.loop(0, hidden_cols // tile)
    def _(c):
        at = pl.ds(pl.multiple_of(c * tile, tile), tile)

        @pl.loop(0, total // tile)
        def _(i):
            here = pl.ds(pl.multiple_of(i * tile, tile), tile)
            gate = jnp.dot(rows_all[here, :], w_gate[:, at], preferred_element_type=F32)
            gate = gate * gate_scale[:, at]
            up = jnp.dot(rows_all[here, :], w_up[:, at], preferred_element_type=F32)
            up = up * up_scale[:, at]
            hidden[here, at] = (gate / (1.0 + jnp.exp(-gate)) * up).astype(BF)

    for k in range(nz):
        for sign in (1, -1) if k else (1,):
            there = coord["z"] + sign * k
            inside = jnp.logical_and(there >= 0, there < nz)

            @pl.when(inside)
            def _():
                product(1, hidden, w_down, fs + sign * k * nx)

    second_line(DOWN, lambda s: product(1, hidden, w_down, s))
    collect(1, residual, result)
    for j in range(1, nt):
        row_copy(1, j, tp).wait_send()
        stat_copy(j, tp).wait_send()

    @pl.loop(0, nf)
    def _(s):
        for j in range(1, nt):
            part_copy(1, j, tp, s).wait_send()

    for allowed, m, s, axis, d in pending:
        pl.when(allowed)(lambda: copy_of(m, s, axis, d).wait_send())


def layer(
    nf, nt,
    tokens, mix_gain, ffn_gain, u_weight, u_scale, v_weight, v_scale, v_gain,
    spatial_weight, spatial_bias, out_weight, out_scale, gate_weight, gate_scale,
    up_weight, up_scale, down_weight, down_scale,
):
    nz = max(n for n in (1, 2, 4) if nf % n == 0)
    nx = nf // nz
    local, width = tokens.shape
    total = local * nt
    cols, ff = u_weight.shape[1], gate_weight.shape[1]
    groups = A_GROUPS // nt
    first = lax.axis_index("tp") * groups
    causal = jnp.tril(jnp.ones((BLK, BLK), dtype=bool))
    mixers = lax.dynamic_slice_in_dim(spatial_weight, first, groups, 0)
    mixers = jnp.where(causal[None], mixers, jnp.zeros_like(mixers))
    offsets = lax.dynamic_slice_in_dim(spatial_bias, first, groups, 0).T
    uv = jnp.concatenate([u_weight.astype(BF), v_weight.astype(BF)], axis=1)
    uv_scale = jnp.concatenate([u_scale, v_scale])[None]
    out = (out_weight * out_scale[None]).astype(BF)
    down = (down_weight * down_scale[None]).astype(BF)
    block = out.shape[1]
    vmem = pl.BlockSpec(memory_space=pltpu.VMEM)
    hbm = pl.BlockSpec(memory_space=pl.ANY)
    dma = pltpu.SemaphoreType.DMA
    return pl.pallas_call(
        functools.partial(kernel, nf, nt, nz, nx),
        out_shape=jax.ShapeDtypeStruct((local, width), BF),
        in_specs=[vmem] * 9 + [hbm] * 5,
        out_specs=vmem,
        scratch_shapes=[
            pltpu.VMEM((width, 2 * cols), BF),
            pltpu.VMEM((nf,) + out.shape, BF),
            pltpu.VMEM((width, ff), BF),
            pltpu.VMEM((width, ff), BF),
            pltpu.VMEM((nf,) + down.shape, BF),
            pltpu.VMEM((total, width), BF),
            pltpu.VMEM((total, cols), BF),
            pltpu.VMEM((total, cols), BF),
            pltpu.VMEM((total, cols), BF),
            pltpu.VMEM((total, ff), BF),
            pltpu.VMEM((nf, total, block), BF),
            pltpu.VMEM((nt, nf, local, block), BF),
            pltpu.VMEM((nt, 8, total), F32),
            pltpu.VMEM((local, width), BF),
            dma((5,)), dma((5, nf)), dma((5, nf, 4)),
            dma((2, nt)), dma((2, nt)), dma((nt,)), dma((nt,)),
            dma((2, nt, nf)), dma((2, nt, nf)),
        ],
        compiler_params=pltpu.CompilerParams(
            has_side_effects=True, vmem_limit_bytes=67043328
        ),
    )(
        tokens, mix_gain[None], ffn_gain[None], uv_scale, v_gain[None], mixers, offsets,
        gate_scale[None], up_scale[None],
        uv, out, gate_weight.astype(BF), up_weight.astype(BF), down,
    )


def solution(mesh):
    placed = (
        P(("fs", "tp"), None), P(), P(),
        P("fs", "tp"), P("tp"), P("fs", "tp"), P("tp"), P("tp"), P(), P(),
        P("tp", "fs"), P("fs"), P("fs", "tp"), P("tp"), P("fs", "tp"), P("tp"),
        P("tp", "fs"), P("fs"),
    )
    return jax.shard_map(
        functools.partial(layer, mesh.shape["fs"], mesh.shape["tp"]),
        mesh=mesh, in_specs=placed, out_specs=P(("fs", "tp"), None), check_vma=False,
    )
```

```python
import functools
import jax
import jax.numpy as jnp
from jax import lax
from jax.experimental import pallas as pl
from jax.experimental.pallas import tpu as pltpu
from jax.sharding import PartitionSpec as P

A_GROUPS = 8
BLK = 128
UV, OUT, GATE, UP, DOWN = (0,), (1,), (2, 3), (4, 5), (6, 7)
PIECES = 8
X_FIRST = ()
BF = jnp.bfloat16
F32 = jnp.float32


def rms(values, gain):
    wide = values.astype(F32)
    factor = lax.rsqrt(jnp.mean(wide * wide, axis=1, keepdims=True) + 1e-06)
    return (wide * factor * gain).astype(BF)


def kernel(
    nf, nt, nz, nx,
    tokens, mix_gain, ffn_gain, u_scale, v_scale, v_gain, mixers, offsets, gate_scale, up_scale,
    uv_in, out_in, gate_in, up_in, down_in,
    result,
    w_uv, w_out, w_gate, w_up, w_down, rows_all, uvals, vvals, gated, hidden, gates,
    staged, landed, stats, residual,
    own_sem, w_recv, w_send, row_recv, row_send, stat_recv, stat_send, part_recv, part_send,
):
    fs, tp = lax.axis_index("fs"), lax.axis_index("tp")
    coord = {"z": fs // nx, "x": fs % nx}
    size = {"z": nz, "x": nx}
    stride = {"z": nx, "x": 1}
    order = {m: ("x", "z") if m in X_FIRST else ("z", "x") for m in range(PIECES)}
    local = tokens.shape[0]
    total = rows_all.shape[0]
    width = tokens.shape[1]
    cols = uvals.shape[1]
    table = {}
    for pieces, source, whole in (
        (UV, uv_in, w_uv), (OUT, out_in, w_out), (GATE, gate_in, w_gate),
        (UP, up_in, w_up), (DOWN, down_in, w_down),
    ):
        for h, m in enumerate(pieces):
            table[m] = (source, whole, h, source.shape[0] // len(pieces))

    def shard(m):
        source, _, h, rows = table[m]
        return source.at[pl.ds(h * rows, rows)]

    def slot(m, s):
        source, whole, h, rows = table[m]
        if m in OUT + DOWN:
            return whole.at[s, pl.ds(h * rows, rows)]
        start = s * source.shape[0] + h * rows
        return whole.at[pl.ds(pl.multiple_of(start, rows), rows)]

    def reaches(axis, d):
        return coord[axis] + d < size[axis] if d > 0 else coord[axis] > 0

    pending = []

    def copy_of(m, s, axis, d):
        lane = (0 if axis == "z" else 2) + (0 if d > 0 else 1)
        return pltpu.make_async_remote_copy(
            src_ref=slot(m, s), dst_ref=slot(m, s),
            send_sem=w_send.at[m, s, lane], recv_sem=w_recv.at[m, s],
            device_id={"fs": fs + d * stride[axis], "tp": tp},
            device_id_type=pl.DeviceIdType.MESH,
        )

    def send(m, s, axis, d, valid):
        allowed = jnp.logical_and(valid, reaches(axis, d))

        @pl.when(allowed)
        def _():
            copy_of(m, s, axis, d).start()

        pending.append((allowed, m, s, axis, d))

    def own(pieces, axis):
        for m in pieces:
            if size[axis] > 1:
                for d in (1, -1):
                    send(m, fs, axis, d, fs >= 0)

    def arrived(m, s, axis, d, valid):
        @pl.when(valid)
        def _():
            copy_of(m, s, axis, -d).wait_recv()

    def first_line(pieces, steps=None):
        p, q = order[pieces[0]]
        for t in range(1, size[p]) if steps is None else steps:
            if t >= size[p]:
                continue
            for m in pieces:
                for d in (1, -1):
                    at = coord[p] - d * t
                    valid = jnp.logical_and(at >= 0, at < size[p])
                    s = jnp.where(valid, fs - d * t * stride[p], fs)
                    arrived(m, s, p, d, valid)
                    if t < size[p] - 1:
                        send(m, s, p, d, valid)
                    if size[q] > 1:
                        for e in (1, -1):
                            send(m, s, q, e, valid)

    def second_line(pieces, steps=None, then=None):
        p, q = order[pieces[0]]
        for k in range(size[p]) if steps is None else steps:
            if k >= size[p]:
                continue
            for sign in (1, -1) if k else (1,):
                there = coord[p] + sign * k
                inside = jnp.logical_and(there >= 0, there < size[p])
                for t in range(1, size[q]):
                    for d in (1, -1):
                        at = coord[q] - d * t
                        valid = jnp.logical_and(inside, jnp.logical_and(at >= 0, at < size[q]))
                        s = jnp.where(valid, fs + sign * k * stride[p] - d * t * stride[q], fs)
                        for m in pieces:
                            arrived(m, s, q, d, valid)
                            if t < size[q] - 1:
                                send(m, s, q, d, valid)
                        if then:
                            pl.when(valid)(functools.partial(then, s))

    mine = [pltpu.make_async_copy(shard(m), slot(m, fs), own_sem.at[m]) for m in range(PIECES)]
    for copy in mine:
        copy.start()

    def ready(pieces):
        for m in pieces:
            mine[m].wait()

    ready(UV)
    own(UV, "z")
    own(UV, "x")

    def peer_of(j):
        return lax.rem(tp + j, nt)

    def row_copy(phase, j, owner):
        part = rows_all.at[pl.ds(pl.multiple_of(owner * local, local), local)]
        return pltpu.make_async_remote_copy(
            src_ref=part, dst_ref=part,
            send_sem=row_send.at[phase, j], recv_sem=row_recv.at[phase, owner],
            device_id={"fs": fs, "tp": peer_of(j)}, device_id_type=pl.DeviceIdType.MESH,
        )

    def stat_copy(j, owner):
        return pltpu.make_async_remote_copy(
            src_ref=stats.at[owner], dst_ref=stats.at[owner],
            send_sem=stat_send.at[j], recv_sem=stat_recv.at[owner],
            device_id={"fs": fs, "tp": peer_of(j)}, device_id_type=pl.DeviceIdType.MESH,
        )

    def part_copy(phase, j, owner, s):
        peer = peer_of(j)
        return pltpu.make_async_remote_copy(
            src_ref=staged.at[s, pl.ds(pl.multiple_of(peer * local, local), local)],
            dst_ref=landed.at[owner, s],
            send_sem=part_send.at[phase, j, s], recv_sem=part_recv.at[phase, owner, s],
            device_id={"fs": fs, "tp": peer}, device_id_type=pl.DeviceIdType.MESH,
        )

    step = min(64, local)

    def norm_rows(source, gain):
        @pl.loop(0, local // step)
        def _(i):
            here = pl.ds(pl.multiple_of(i * step, step), step)
            there = pl.ds(pl.multiple_of(tp * local + i * step, step), step)
            rows_all[there, :] = rms(source[here, :], gain[...][None])

    norm_rows(tokens, mix_gain)
    for j in range(1, nt):
        row_copy(0, j, tp).start()
    ready(OUT)
    own(OUT, "x")
    own(OUT, "z")
    ready(GATE)
    own(GATE, "x")
    first_line(UV)
    own(GATE, "z")
    ready(UP)
    own(UP, "x")
    second_line(UV)
    for j in range(1, nt):
        row_copy(0, j, peer_of(j)).wait_recv()

    first_line(OUT, (1, 2))
    tile = 256
    stat_rows = BLK

    @pl.loop(0, total // tile)
    def _(i):
        here = pl.ds(pl.multiple_of(i * tile, tile), tile)
        for c in range(2 * cols // tile):
            at = slice(c * tile, (c + 1) * tile)
            pre = jnp.dot(rows_all[here, :], w_uv[:, at], preferred_element_type=F32)
            scale, away = (u_scale, 0) if c * tile < cols else (v_scale, cols)
            pre = pre * scale[c * tile - away:(c + 1) * tile - away][None]
            value = jax.nn.gelu(pre, approximate=True).astype(BF)
            if c * tile < cols:
                uvals[here, at] = value
            else:
                vvals[here, c * tile - cols:(c + 1) * tile - cols] = value

    lanes = lax.broadcasted_iota(jnp.int32, (stat_rows, 128), 1)

    @pl.loop(0, total // stat_rows)
    def _(i):
        here = pl.ds(pl.multiple_of(i * stat_rows, stat_rows), stat_rows)
        wide = vvals[here, :].astype(F32)
        sums = jnp.sum(wide, axis=1, keepdims=True)
        squares = jnp.sum(wide * wide, axis=1, keepdims=True)
        both = jnp.where(lanes == 0, sums, jnp.where(lanes == 1, squares, 0.0))
        stats[tp, :, here] = both.T[0:8, :]

    for j in range(1, nt):
        stat_copy(j, tp).start()
    first_line(OUT, range(3, nz))
    own(UP, "z")
    ready(DOWN)
    own(DOWN, "x")
    second_line(OUT)
    for j in range(1, nt):
        stat_copy(j, peer_of(j)).wait_recv()

    causal = (
        lax.broadcasted_iota(jnp.int32, (BLK, BLK), 0)
        >= lax.broadcasted_iota(jnp.int32, (BLK, BLK), 1)
    )
    groups = A_GROUPS // nt
    group_dim = (cols * nt) // A_GROUPS

    @pl.loop(0, total // BLK)
    def _(i):
        here = pl.ds(pl.multiple_of(i * BLK, BLK), BLK)
        summed = stats[0, :, here]
        for t in range(1, nt):
            summed = summed + stats[t, :, here]
        turned = jnp.concatenate([summed] * (BLK // 8), axis=0).T
        average = turned[:, 0:1] / (cols * nt)
        spread = turned[:, 1:2] / (cols * nt) - average * average
        wide = vvals[here, :].astype(F32)
        normed = ((wide - average) * lax.rsqrt(spread + 1e-05) * v_gain[...][None]).astype(BF)
        for g in range(cols // group_dim):
            at = slice(g * group_dim, (g + 1) * group_dim)
            weights = mixers[tp * groups + g].astype(F32)
            weights = jnp.where(causal, weights, 0.0).astype(BF)
            mixed = jnp.dot(weights, normed[:, at], preferred_element_type=F32)
            mixed = mixed + offsets[:, g:g + 1]
            gated[here, at] = (uvals[here, at].astype(F32) * mixed).astype(BF)

    def product(phase, left, matrix, s):
        part = min(512, total)

        @pl.loop(0, total // part)
        def _(i):
            here = pl.ds(pl.multiple_of(i * part, part), part)
            staged[s, here, :] = jnp.dot(
                left[here, :], matrix[s], preferred_element_type=F32
            ).astype(BF)

        for j in range(1, nt):
            part_copy(phase, j, tp, s).start()

    @pl.loop(0, nf)
    def _(s):
        product(0, gated, w_out, s)

    first_line(GATE)
    own(DOWN, "z")

    block = staged.shape[2]

    def collect(phase, base, target):
        for s in range(nf):
            for j in range(1, nt):
                part_copy(phase, j, peer_of(j), s).wait_recv()
            at = slice(s * block, (s + 1) * block)
            summed = staged[s, pl.ds(pl.multiple_of(tp * local, local), local), :].astype(F32)
            for j in range(1, nt):
                summed = summed + landed[peer_of(j), s].astype(F32)
            target[:, at] = (base[:, at].astype(F32) + summed).astype(BF)

    collect(0, tokens, residual)
    for j in range(1, nt):
        row_copy(0, j, tp).wait_send()
    norm_rows(residual, ffn_gain)
    for j in range(1, nt):
        row_copy(1, j, tp).start()
    first_line(UP, (1,))

    @pl.loop(0, nf)
    def _(s):
        for j in range(1, nt):
            part_copy(0, j, tp, s).wait_send()

    second_line(GATE)
    first_line(UP, (2,))
    for j in range(1, nt):
        row_copy(1, j, peer_of(j)).wait_recv()
    hidden_cols = hidden.shape[1]
    part = min(512, total)

    def each_tile(body):
        @pl.loop(0, hidden_cols // tile)
        def _(c):
            at = pl.ds(pl.multiple_of(c * tile, tile), tile)

            @pl.loop(0, total // part)
            def _(i):
                body(pl.ds(pl.multiple_of(i * part, part), part), at)

    def gate_tile(here, at):
        gate = jnp.dot(rows_all[here, :], w_gate[:, at], preferred_element_type=F32)
        gate = gate * gate_scale[at][None]
        gates[here, at] = gate / (1.0 + jnp.exp(-gate))

    def up_tile(here, at):
        up = jnp.dot(rows_all[here, :], w_up[:, at], preferred_element_type=F32)
        hidden[here, at] = (gates[here, at] * (up * up_scale[at][None])).astype(BF)

    each_tile(gate_tile)
    first_line(UP, range(3, nz))
    first_line(DOWN, (1,))
    second_line(UP)
    each_tile(up_tile)

    def down_of(s):
        product(1, hidden, w_down, s)

    for k in range(nz):
        if k:
            first_line(DOWN, (k + 1,))
        for sign in (1, -1) if k else (1,):
            there = coord["z"] + sign * k
            inside = jnp.logical_and(there >= 0, there < nz)
            pl.when(inside)(functools.partial(down_of, fs + sign * k * nx))
        second_line(DOWN, (k,), down_of)

    collect(1, residual, result)
    for j in range(1, nt):
        row_copy(1, j, tp).wait_send()
        stat_copy(j, tp).wait_send()

    @pl.loop(0, nf)
    def _(s):
        for j in range(1, nt):
            part_copy(1, j, tp, s).wait_send()

    for allowed, m, s, axis, d in pending:
        pl.when(allowed)(lambda: copy_of(m, s, axis, d).wait_send())


def layer(
    nf, nt,
    tokens, mix_gain, ffn_gain, u_weight, u_scale, v_weight, v_scale, v_gain,
    spatial_weight, spatial_bias, out_weight, out_scale, gate_weight, gate_scale,
    up_weight, up_scale, down_weight, down_scale,
):
    nz = max(n for n in (1, 2, 4) if nf % n == 0)
    nx = nf // nz
    local, width = tokens.shape
    total = local * nt
    cols, ff = u_weight.shape[1], gate_weight.shape[1]
    groups = A_GROUPS // nt
    first = lax.axis_index("tp") * groups
    offsets = lax.dynamic_slice_in_dim(spatial_bias, first, groups, 0).T
    uv = jnp.concatenate([u_weight.astype(BF), v_weight.astype(BF)], axis=1)
    out = (out_weight * out_scale[None]).astype(BF)
    down = (down_weight * down_scale[None]).astype(BF)
    block = out.shape[1]
    vmem = pl.BlockSpec(memory_space=pltpu.VMEM)
    hbm = pl.BlockSpec(memory_space=pl.ANY)
    dma = pltpu.SemaphoreType.DMA
    return pl.pallas_call(
        functools.partial(kernel, nf, nt, nz, nx),
        out_shape=jax.ShapeDtypeStruct((local, width), BF),
        in_specs=[vmem] * 10 + [hbm] * 5,
        out_specs=vmem,
        scratch_shapes=[
            pltpu.VMEM((width, 2 * cols), BF),
            pltpu.VMEM((nf,) + out.shape, BF),
            pltpu.VMEM((width, ff), BF),
            pltpu.VMEM((width, ff), BF),
            pltpu.VMEM((nf,) + down.shape, BF),
            pltpu.VMEM((total, width), BF),
            pltpu.VMEM((total, cols), BF),
            pltpu.VMEM((total, cols), BF),
            pltpu.VMEM((total, cols), BF),
            pltpu.VMEM((total, ff), BF),
            pltpu.VMEM((total, ff), F32),
            pltpu.VMEM((nf, total, block), BF),
            pltpu.VMEM((nt, nf, local, block), BF),
            pltpu.VMEM((nt, 8, total), F32),
            pltpu.VMEM((local, width), BF),
            dma((PIECES,)), dma((PIECES, nf)), dma((PIECES, nf, 4)),
            dma((2, nt)), dma((2, nt)), dma((nt,)), dma((nt,)),
            dma((2, nt, nf)), dma((2, nt, nf)),
        ],
        compiler_params=pltpu.CompilerParams(
            has_side_effects=True, vmem_limit_bytes=67043328
        ),
    )(
        tokens, mix_gain, ffn_gain, u_scale, v_scale, v_gain, spatial_weight, offsets,
        gate_scale, up_scale,
        uv, out, gate_weight.astype(BF), up_weight.astype(BF), down,
    )


def solution(mesh):
    placed = (
        P(("fs", "tp"), None), P(), P(),
        P("fs", "tp"), P("tp"), P("fs", "tp"), P("tp"), P("tp"), P(), P(),
        P("tp", "fs"), P("fs"), P("fs", "tp"), P("tp"), P("fs", "tp"), P("tp"),
        P("tp", "fs"), P("fs"),
    )
    return jax.shard_map(
        functools.partial(layer, mesh.shape["fs"], mesh.shape["tp"]),
        mesh=mesh, in_specs=placed, out_specs=P(("fs", "tp"), None), check_vma=False,
    )
```
